32 devices in a mesh: gr: 2 (over x), fs: 8 (over z, y), tp: 2 (over core).
Axes of the slice: x: 2, y: 2, z: 4, core: 2. Of those that a mesh axis runs over, the one named last changes fastest.
Arguments:
- tokens: bfloat16 [4096, 2048], P(('gr', 'fs', 'tp')), may hold values from -6 to 6
- norm_gain: float32 [2048], P(('gr', 'fs')), may hold values from 0.1 to 1.9
- up_weight: float32 [2048, 8192], P(('gr', 'fs'), 'tp'), may hold values from -0.125 to 0.125
- down_weight: float32 [8192, 2048], P(('gr', 'fs'), 'tp'), may hold values from -0.0625 to 0.0625
Outputs:
- served: bfloat16 [4096, 2048], P(('gr', 'fs', 'tp'))
- serve_up: bfloat16 [2048, 8192], P(None, 'fs')
- serve_down: bfloat16 [8192, 2048], P('fs')
The draws below stay inside these ranges and needn't reach their ends.
All inputs are finite; a program needn't handle non-finite values.
Results may differ from the reference program's by a relative error of at most 0.017.
Values may be sent and summed in bfloat16 or wider, within the bound.
A program may use at most 64 MiB of HBM per device.

```python
import jax
import jax.numpy as jnp
from jax import lax

D = 2048
FF = 8192
TOKENS = 4096
N_GR = 2
N_FS = 8


def level_of(stream_key, shape, pieces, least, top_value):
    factor_of = 1.0
    for position, blocks in pieces:
        draws = jax.random.uniform(jax.random.fold_in(jax.random.fold_in(stream_key, 6), position), (blocks,), jnp.float32, least / len(pieces), top_value / len(pieces))
        factor_of = factor_of * jnp.repeat(jnp.exp(draws), shape[position] // blocks).reshape((-1,) + (1,) * (len(shape) - 1 - position))
    return factor_of


def noise(key, dims, spread, reach, split=(), dtype=jnp.bfloat16):
    array = jax.random.normal(key, dims, jnp.float32) * spread
    if len(split) > 0:
        array = level_of(key, dims, split, -0.22, 0.18) * array
    return jnp.clip(array, min=-reach, max=reach).astype(dtype)


def setup_inputs(seed: int = 0) -> dict:
    key_list = jax.random.split(jax.random.key(seed), 5)
    return {
        "tokens": noise(key_list[0], (TOKENS, D), 1.0, 6.0, ((0, 32),)),
        "norm_gain": jnp.clip(1.0 + 0.18 * jax.random.normal(key_list[1], (D,), jnp.float32), 0.1, 1.9),
        "up_weight": noise(key_list[2], (D, FF), D ** -0.5, 0.125, ((0, 16), (1, 2)), jnp.float32),
        "down_weight": noise(key_list[3], (FF, D), FF ** -0.5, 0.0625, ((0, 16), (1, 2)), jnp.float32),
    }


def reference(tokens, norm_gain, up_weight, down_weight):
    segment = FF // (N_GR * N_FS)
    block = FF // N_FS
    scaled = (norm_gain[:, None] * up_weight).astype(jnp.bfloat16)
    serve_up = scaled.reshape(D, N_GR, N_FS, segment).transpose(0, 2, 1, 3).reshape(D, FF)
    rounded = down_weight.astype(jnp.bfloat16)
    serve_down = rounded.reshape(N_GR, N_FS, segment, D).transpose(1, 0, 2, 3).reshape(FF, D)
    values = tokens.astype(jnp.float32)
    normed = (values * lax.rsqrt(lax.optimization_barrier(jnp.mean(values * values, axis=1, keepdims=True)) + 1e-06)).astype(jnp.bfloat16)
    hidden = jnp.square(jax.nn.relu(jnp.dot(normed, serve_up, preferred_element_type=jnp.float32))).astype(jnp.bfloat16)
    hidden_blocks = hidden.reshape(hidden.shape[0], N_FS, block).transpose(1, 0, 2)
    down_blocks = serve_down.reshape(N_FS, block, D)

    def accumulate(total, pair):
        part = jnp.dot(pair[0], pair[1], preferred_element_type=jnp.float32).astype(jnp.bfloat16)
        part = lax.optimization_barrier(part)
        return (total + part.astype(jnp.float32), None)
    total, unused = lax.scan(accumulate, jnp.zeros((hidden.shape[0], D), jnp.float32), (hidden_blocks, down_blocks))
    return (total.astype(jnp.bfloat16), serve_up, serve_down)
```

```python
import functools

import jax
import jax.numpy as jnp
from jax import lax
from jax.experimental import pallas as pl
from jax.experimental.pallas import tpu as pltpu
from jax.sharding import PartitionSpec as P

MESH = pl.DeviceIdType.MESH
TILE = 256


def kernel(sizes, normed, up, down, served, out_up, out_down, tok, su, sd, hid, part, got, *sems):
    groups, shards, cores = sizes
    (up_send, up_recv, gu_send, gu_recv, tu_send, tu_recv, gd_send, gd_recv,
     td_send, td_recv, tok_send, tok_recv, part_send, part_recv, local, out_sem) = sems
    g, f, t = lax.axis_index("gr"), lax.axis_index("fs"), lax.axis_index("tp")
    rows, depth = normed.shape
    own_rows = up.shape[0]
    segment, dcols = down.shape
    nseg = up.shape[1] // segment
    group_rows = shards * own_rows

    def to(axis, me, size, step):
        return {axis: lax.rem(me + step, size)}

    def rdma(src, dst, send, recv, device):
        return pltpu.make_async_remote_copy(
            src_ref=src, dst_ref=dst, send_sem=send, recv_sem=recv,
            device_id=device, device_id_type=MESH,
        )

    peers = [to("fs", f, shards, k) for k in range(1, shards)]
    peers += [to("gr", g, groups, k) for k in range(1, groups)]
    peers += [to("tp", t, cores, k) for k in range(1, cores)]
    barrier = pltpu.get_barrier_semaphore()
    for peer in peers:
        pl.semaphore_signal(barrier, inc=1, device_id=peer, device_id_type=MESH)
    pl.semaphore_wait(barrier, len(peers))

    def up_block(group, shard, sg):
        row = pl.multiple_of((group * shards + shard) * own_rows, own_rows)
        return su.at[pl.ds(row, own_rows), pl.ds(pl.multiple_of(sg * segment, segment), segment)]

    def up_group(group, sg):
        row = pl.multiple_of(group * group_rows, group_rows)
        return su.at[pl.ds(row, group_rows), pl.ds(sg * segment, segment)]

    def down_block(group, core):
        row = pl.multiple_of(group * segment, segment)
        return sd.at[pl.ds(row, segment), pl.ds(pl.multiple_of(core * dcols, dcols), dcols)]

    def owner(sg):
        return (sg * shards + f) // nseg

    def up_copy(i):
        number = t * nseg + i
        shard, sg = lax.rem(number, shards), number // shards
        step = lax.rem(shard - f + shards, shards)
        src = up.at[:, pl.ds(pl.multiple_of(i * segment, segment), segment)]
        remote = rdma(src, up_block(g, f, sg), up_send.at[i], up_recv.at[sg, step], {"fs": shard})
        here = pltpu.make_async_copy(src, up_block(g, f, sg), up_recv.at[sg, 0])
        return shard == f, here, remote

    def start_up(j, carry):
        mine, here, remote = up_copy(lax.rem(f + j, nseg))
        pl.when(mine)(here.start)
        pl.when(jnp.logical_not(mine))(remote.start)
        return carry

    lax.fori_loop(0, nseg, start_up, 0)

    sends = []
    keep_down = pltpu.make_async_copy(down, down_block(g, t), local.at[0])
    keep_tok = pltpu.make_async_copy(normed, tok.at[pl.ds((shards - 1) * rows, rows)], local.at[1])
    keep_down.start()
    keep_tok.start()
    down_in = []
    for k in range(1, groups):
        copy = rdma(down, down_block(g, t), gd_send.at[k], gd_recv.at[k], to("gr", g, groups, k))
        copy.start()
        sends.append(copy)
        source = lax.rem(g + groups - k, groups)
        down_in.append((k, source))
    for k in range(1, cores):
        copy = rdma(down, down_block(g, t), td_send.at[k, 0], td_recv.at[k, 0], to("tp", t, cores, k))
        copy.start()
        sends.append(copy)

    for k in range(1, shards):
        copy = rdma(normed, tok.at[pl.ds((k - 1) * rows, rows)], tok_send.at[k], tok_recv.at[k],
                    to("fs", f, shards, k))
        copy.start()
        sends.append(copy)

    for sg in range(groups):
        def forward(sg=sg):
            def arrived(k, carry):
                shard = lax.rem(f + shards - k, shards)
                block = up_block(g, shard, sg)
                if True:
                    @pl.when(k == 0)
                    def _():
                        pltpu.make_async_copy(block, block, up_recv.at[sg, 0]).wait()

                    @pl.when(k > 0)
                    def _():
                        rdma(block, block, up_send.at[0], up_recv.at[sg, k], {"fs": shard}).wait_recv()
                for d in range(1, groups):
                    rdma(block, block, gu_send.at[sg, d, k], gu_recv.at[sg, d, k],
                         to("gr", g, groups, d)).start()
                return carry

            lax.fori_loop(0, shards, arrived, 0)
            whole = up_group(g, sg)
            for c in range(1, cores):
                rdma(whole, whole, tu_send.at[sg, 0, c], tu_recv.at[sg, 0], to("tp", t, cores, c)).start()

        pl.when(owner(sg) == t)(forward)

    for k, source in down_in:
        block = down_block(source, t)
        rdma(block, block, gd_send.at[k], gd_recv.at[k], {"gr": source}).wait_recv()
        for c in range(1, cores):
            copy = rdma(block, block, td_send.at[c, k], td_recv.at[c, k], to("tp", t, cores, c))
            copy.start()
            sends.append(copy)

    for sg in range(groups):
        def onward(sg=sg):
            for d in range(1, groups):
                source = lax.rem(g + groups - d, groups)

                def arrived(k, carry):
                    block = up_block(source, lax.rem(f + shards - k, shards), sg)
                    rdma(block, block, gu_send.at[sg, d, k], gu_recv.at[sg, d, k], {"gr": source}).wait()
                    return carry

                lax.fori_loop(0, shards, arrived, 0)
                whole = up_group(source, sg)
                for c in range(1, cores):
                    rdma(whole, whole, tu_send.at[sg, d, c], tu_recv.at[sg, d],
                         to("tp", t, cores, c)).start()

        pl.when(owner(sg) == t)(onward)

    keep_down.wait()
    keep_tok.wait()
    for c in range(1, cores):
        core = lax.rem(t + cores - c, cores)
        for k in range(groups):
            block = down_block(lax.rem(g + groups - k, groups), core)
            rdma(block, block, td_send.at[c, k], td_recv.at[c, k], {"tp": core}).wait_recv()
    for sg in range(groups):
        def take(sg=sg):
            for d in range(groups):
                whole = up_group(lax.rem(g + groups - d, groups), sg)
                rdma(whole, whole, tu_send.at[sg, d, 1], tu_recv.at[sg, d],
                     {"tp": owner(sg)}).wait_recv()

        pl.when(owner(sg) != t)(take)

    put_up = pltpu.make_async_copy(su, out_up, out_sem.at[0])
    put_down = pltpu.make_async_copy(sd, out_down, out_sem.at[1])
    put_up.start()
    put_down.start()

    def part_copy(k):
        at = pl.ds(pl.multiple_of((k - 1) * rows, rows), rows)
        return rdma(part.at[at], got.at[at], part_send.at[k], part_recv.at[k],
                    {"fs": lax.rem(f + shards - k, shards)})

    width = su.shape[1]

    def pair(j, carry):
        for k in (2 * j + 1, 2 * j + 2):
            at = pl.ds(pl.multiple_of((k - 1) * rows, rows), rows)

            @pl.when(k < shards)
            def _():
                rdma(normed, tok.at[at], tok_send.at[k], tok_recv.at[k],
                     {"fs": lax.rem(f + shards - k, shards)}).wait_recv()

        both = pl.ds(pl.multiple_of(2 * j * rows, 2 * rows), 2 * rows)

        def first(n, carry):
            cols = pl.ds(pl.multiple_of(n * TILE, TILE), TILE)
            product = jnp.dot(tok[both, :], su[:, cols], preferred_element_type=jnp.float32)
            product = jnp.maximum(product, 0.0)
            hid[:, cols] = (product * product).astype(jnp.bfloat16)
            return carry

        lax.fori_loop(0, width // TILE, first, 0)

        def second(n, carry):
            cols = pl.ds(pl.multiple_of(n * TILE, TILE), TILE)
            product = jnp.dot(hid[...], sd[:, cols], preferred_element_type=jnp.float32)
            part[both, cols] = product.astype(jnp.bfloat16)
            return carry

        lax.fori_loop(0, depth // TILE, second, 0)
        for k in (2 * j + 1, 2 * j + 2):
            @pl.when(k < shards)
            def _():
                part_copy(k).start()
        return carry

    lax.fori_loop(0, shards // 2, pair, 0)

    def finish(k, carry):
        part_copy(k).wait()
        return carry

    lax.fori_loop(1, shards, finish, 0)

    def total(r, carry):
        at = pl.multiple_of(r * 16, 16)
        value = part[pl.ds((shards - 1) * rows + at, 16), :].astype(jnp.float32)
        for k in range(1, shards):
            value += got[pl.ds((k - 1) * rows + at, 16), :].astype(jnp.float32)
        served[pl.ds(at, 16), :] = value.astype(jnp.bfloat16)
        return carry

    lax.fori_loop(0, rows // 16, total, 0)

    for copy in sends:
        copy.wait_send()

    def end_up(j, carry):
        mine, here, remote = up_copy(j)
        pl.when(jnp.logical_not(mine))(remote.wait_send)
        return carry

    lax.fori_loop(0, nseg, end_up, 0)
    for sg in range(groups):
        def end(sg=sg):
            for d in range(groups):
                whole = up_group(lax.rem(g + groups - d, groups), sg)
                for c in range(1, cores):
                    rdma(whole, whole, tu_send.at[sg, d, c], tu_recv.at[sg, d],
                         to("tp", t, cores, c)).wait_send()

        pl.when(owner(sg) == t)(end)
    put_up.wait()
    put_down.wait()


def body(tokens, norm_gain, up_weight, down_weight):
    groups, shards, cores = (lax.axis_size(a) for a in ("gr", "fs", "tp"))
    segment = down_weight.shape[0]
    up = (norm_gain[:, None] * up_weight).astype(jnp.bfloat16)
    down = down_weight.astype(jnp.bfloat16)
    values = tokens.astype(jnp.float32)
    normed = (values * lax.rsqrt(jnp.mean(values * values, axis=1, keepdims=True) + 1e-06)).astype(
        jnp.bfloat16
    )
    rows, depth = tokens.shape
    nseg = up.shape[1] // segment
    width = groups * segment
    bf = jnp.bfloat16
    dma = pltpu.SemaphoreType.DMA
    vmem = pl.BlockSpec(memory_space=pltpu.VMEM)
    hbm = pl.BlockSpec(memory_space=pl.ANY)
    return pl.pallas_call(
        functools.partial(kernel, (groups, shards, cores)),
        out_shape=(
            jax.ShapeDtypeStruct((rows, depth), bf),
            jax.ShapeDtypeStruct((depth, width), bf),
            jax.ShapeDtypeStruct((width, depth), bf),
        ),
        in_specs=[vmem] * 3,
        out_specs=(vmem, hbm, hbm),
        scratch_shapes=[
            pltpu.VMEM((shards * rows, depth), bf),
            pltpu.VMEM((depth, width), bf),
            pltpu.VMEM((width, depth), bf),
            pltpu.VMEM((2 * rows, width), bf),
            pltpu.VMEM((shards * rows, depth), bf),
            pltpu.VMEM((shards * rows, depth), bf),
            dma((nseg,)), dma((groups, shards)),
            dma((groups, groups, shards)), dma((groups, groups, shards)),
            dma((groups, groups, cores)), dma((groups, groups)),
            dma((groups,)), dma((groups,)),
            dma((cores, groups)), dma((cores, groups)),
            dma((shards,)), dma((shards,)),
            dma((shards,)), dma((shards,)),
            dma((2,)), dma((2,)),
        ],
        compiler_params=pltpu.CompilerParams(
            collective_id=0, has_side_effects=True, vmem_limit_bytes=48 * 1024 * 1024
        ),
        name="serve",
    )(normed, up, down)


def solution(mesh):
    return jax.shard_map(
        body,
        mesh=mesh,
        in_specs=(
            P(("gr", "fs", "tp"), None),
            P(("gr", "fs")),
            P(("gr", "fs"), "tp"),
            P(("gr", "fs"), "tp"),
        ),
        out_specs=(P(("gr", "fs", "tp"), None), P(None, "fs"), P("fs", None)),
        check_vma=False,
    )
```

```python
import functools

import jax
import jax.numpy as jnp
from jax import lax
from jax.experimental import pallas as pl
from jax.experimental.pallas import tpu as pltpu
from jax.sharding import PartitionSpec as P

MESH = pl.DeviceIdType.MESH
TILE = 256


def inner_size(shards):
    return max(d for d in range(1, shards + 1) if shards % d == 0 and d * d <= shards)


def kernel(sizes, normed, up, down, served, out_up, out_down, tok, su, sd, hid, part, got, far, *sems):
    groups, shards, cores = sizes
    inner = inner_size(shards)
    outer = shards // inner
    (up_send, up_recv, gu_send, gu_recv, tu_send, tu_recv, gd_send, gd_recv,
     td_send, td_recv, tok_send, tok_recv, part_send, part_recv, far_send, far_recv, local, out_sem) = sems
    g, f, t = lax.axis_index("gr"), lax.axis_index("fs"), lax.axis_index("tp")
    z, y = f // inner, lax.rem(f, inner)
    rows, depth = normed.shape
    own_rows = up.shape[0]
    segment, dcols = down.shape
    nseg = up.shape[1] // segment
    group_rows = shards * own_rows

    def to(axis, me, size, step):
        return {axis: lax.rem(me + step, size)}

    def rdma(src, dst, send, recv, device):
        return pltpu.make_async_remote_copy(
            src_ref=src, dst_ref=dst, send_sem=send, recv_sem=recv,
            device_id=device, device_id_type=MESH,
        )

    def back(o, i):
        return {"fs": lax.rem(z + outer - o, outer) * inner + lax.rem(y + inner - i, inner)}

    def ahead(o, i):
        return {"fs": lax.rem(z + o, outer) * inner + lax.rem(y + i, inner)}

    def block_of(ref, number, count=1):
        return ref.at[pl.ds(pl.multiple_of(number * rows, rows), count * rows)]

    peers = [to("fs", f, shards, k) for k in range(1, shards)]
    peers += [to("gr", g, groups, k) for k in range(1, groups)]
    peers += [to("tp", t, cores, k) for k in range(1, cores)]
    barrier = pltpu.get_barrier_semaphore()
    for peer in peers:
        pl.semaphore_signal(barrier, inc=1, device_id=peer, device_id_type=MESH)
    pl.semaphore_wait(barrier, len(peers))

    def up_block(group, shard, sg):
        row = pl.multiple_of((group * shards + shard) * own_rows, own_rows)
        return su.at[pl.ds(row, own_rows), pl.ds(pl.multiple_of(sg * segment, segment), segment)]

    def up_group(group, sg):
        row = pl.multiple_of(group * group_rows, group_rows)
        return su.at[pl.ds(row, group_rows), pl.ds(sg * segment, segment)]

    def down_block(group, core):
        row = pl.multiple_of(group * segment, segment)
        return sd.at[pl.ds(row, segment), pl.ds(pl.multiple_of(core * dcols, dcols), dcols)]

    def owner(sg):
        return (sg * shards + f) // nseg

    def up_copy(i):
        number = t * nseg + i
        shard, sg = lax.rem(number, shards), number // shards
        step = lax.rem(shard - f + shards, shards)
        src = up.at[:, pl.ds(pl.multiple_of(i * segment, segment), segment)]
        remote = rdma(src, up_block(g, f, sg), up_send.at[i], up_recv.at[sg, step], {"fs": shard})
        here = pltpu.make_async_copy(src, up_block(g, f, sg), up_recv.at[sg, 0])
        return shard == f, here, remote

    def start_up(j, carry):
        mine, here, remote = up_copy(lax.rem(f + j, nseg))
        pl.when(mine)(here.start)
        pl.when(jnp.logical_not(mine))(remote.start)
        return carry

    lax.fori_loop(0, nseg, start_up, 0)

    sends = []
    keep_down = pltpu.make_async_copy(down, down_block(g, t), local.at[0])
    keep_tok = pltpu.make_async_copy(normed, block_of(tok, 0), local.at[1])
    keep_down.start()
    keep_tok.start()
    down_in = []
    for k in range(1, groups):
        copy = rdma(down, down_block(g, t), gd_send.at[k], gd_recv.at[k], to("gr", g, groups, k))
        copy.start()
        sends.append(copy)
        source = lax.rem(g + groups - k, groups)
        down_in.append((k, source))
    for k in range(1, cores):
        copy = rdma(down, down_block(g, t), td_send.at[k, 0], td_recv.at[k, 0], to("tp", t, cores, k))
        copy.start()
        sends.append(copy)

    for o, i in [(o, 0) for o in range(1, outer)] + [(0, i) for i in range(1, inner)]:
        n = o * inner + i
        copy = rdma(normed, block_of(tok, n), tok_send.at[n], tok_recv.at[n], ahead(o, i))
        copy.start()
        sends.append(copy)

    for sg in range(groups):
        def forward(sg=sg):
            def arrived(k, carry):
                shard = lax.rem(f + shards - k, shards)
                block = up_block(g, shard, sg)

                @pl.when(k == 0)
                def _():
                    pltpu.make_async_copy(block, block, up_recv.at[sg, 0]).wait()

                @pl.when(k > 0)
                def _():
                    rdma(block, block, up_send.at[0], up_recv.at[sg, k], {"fs": shard}).wait_recv()

                for d in range(1, groups):
                    rdma(block, block, gu_send.at[sg, d, k], gu_recv.at[sg, d, k],
                         to("gr", g, groups, d)).start()
                return carry

            lax.fori_loop(0, shards, arrived, 0)
            whole = up_group(g, sg)
            for c in range(1, cores):
                rdma(whole, whole, tu_send.at[sg, 0, c], tu_recv.at[sg, 0], to("tp", t, cores, c)).start()

        pl.when(owner(sg) == t)(forward)

    for o in range(1, outer):
        block = block_of(tok, o * inner)
        rdma(block, block, tok_send.at[o * inner], tok_recv.at[o * inner], back(o, 0)).wait_recv()
        for i in range(1, inner):
            n = o * inner + i
            copy = rdma(block, block_of(tok, n), tok_send.at[n], tok_recv.at[n], ahead(0, i))
            copy.start()
            sends.append(copy)

    for k, source in down_in:
        block = down_block(source, t)
        rdma(block, block, gd_send.at[k], gd_recv.at[k], {"gr": source}).wait_recv()
        for c in range(1, cores):
            copy = rdma(block, block, td_send.at[c, k], td_recv.at[c, k], to("tp", t, cores, c))
            copy.start()
            sends.append(copy)

    for sg in range(groups):
        def onward(sg=sg):
            for d in range(1, groups):
                source = lax.rem(g + groups - d, groups)

                def arrived(k, carry):
                    block = up_block(source, lax.rem(f + shards - k, shards), sg)
                    rdma(block, block, gu_send.at[sg, d, k], gu_recv.at[sg, d, k], {"gr": source}).wait()
                    return carry

                lax.fori_loop(0, shards, arrived, 0)
                whole = up_group(source, sg)
                for c in range(1, cores):
                    rdma(whole, whole, tu_send.at[sg, d, c], tu_recv.at[sg, d],
                         to("tp", t, cores, c)).start()

        pl.when(owner(sg) == t)(onward)

    keep_down.wait()
    keep_tok.wait()
    for c in range(1, cores):
        core = lax.rem(t + cores - c, cores)
        for k in range(groups):
            block = down_block(lax.rem(g + groups - k, groups), core)
            rdma(block, block, td_send.at[c, k], td_recv.at[c, k], {"tp": core}).wait_recv()
    for sg in range(groups):
        def take(sg=sg):
            for d in range(groups):
                whole = up_group(lax.rem(g + groups - d, groups), sg)
                rdma(whole, whole, tu_send.at[sg, d, 1], tu_recv.at[sg, d],
                     {"tp": owner(sg)}).wait_recv()

        pl.when(owner(sg) != t)(take)

    put_up = pltpu.make_async_copy(su, out_up, out_sem.at[0])
    put_down = pltpu.make_async_copy(sd, out_down, out_sem.at[1])
    put_up.start()
    put_down.start()

    width = su.shape[1]
    stack = inner * rows

    def near_copy(o, i):
        n = o * inner + i
        return rdma(block_of(part, n), block_of(got, n), part_send.at[n], part_recv.at[n], back(0, i))

    def far_copy(o):
        return rdma(block_of(part, o * inner), block_of(far, o), far_send.at[o], far_recv.at[o], back(o, 0))

    def compute(o):
        for i in range(1, inner):
            block = block_of(tok, o * inner + i)
            n = o * inner + i
            rdma(block, block, tok_send.at[n], tok_recv.at[n], back(0, i)).wait_recv()
        both = pl.ds(pl.multiple_of(o * stack, stack), stack)

        def first(n, carry):
            cols = pl.ds(pl.multiple_of(n * TILE, TILE), TILE)
            product = jnp.dot(tok[both, :], su[:, cols], preferred_element_type=jnp.float32)
            product = jnp.maximum(product, 0.0)
            hid[:, cols] = (product * product).astype(jnp.bfloat16)
            return carry

        lax.fori_loop(0, width // TILE, first, 0)

        def second(n, carry):
            cols = pl.ds(pl.multiple_of(n * TILE, TILE), TILE)
            product = jnp.dot(hid[...], sd[:, cols], preferred_element_type=jnp.float32)
            part[both, cols] = product.astype(jnp.bfloat16)
            return carry

        lax.fori_loop(0, depth // TILE, second, 0)
        for i in range(1, inner):
            near_copy(o, i).start()

    def gather(o):
        for i in range(1, inner):
            near_copy(o, i).wait()

    def add(o):
        gather(o)

        def chunk(r, carry):
            at = pl.multiple_of(r * 16, 16)
            mine = pl.ds(pl.multiple_of(o * stack + at, 16), 16)
            value = part[mine, :].astype(jnp.float32)
            for i in range(1, inner):
                value += got[pl.ds(pl.multiple_of(o * stack + i * rows + at, 16), 16), :].astype(jnp.float32)
            part[mine, :] = value.astype(jnp.bfloat16)
            return carry

        lax.fori_loop(0, rows // 16, chunk, 0)
        far_copy(o).start()

    def step(o, carry):
        compute(lax.rem(o, outer))
        pl.when(o > 1)(lambda: add(o - 1))
        return carry

    lax.fori_loop(1, outer + 1, step, 0)
    gather(0)

    def finish(o, carry):
        far_copy(o).wait()
        return carry

    lax.fori_loop(1, outer, finish, 0)

    def total(r, carry):
        at = pl.multiple_of(r * 16, 16)
        value = part[pl.ds(at, 16), :].astype(jnp.float32)
        for i in range(1, inner):
            value += got[pl.ds(pl.multiple_of(i * rows + at, 16), 16), :].astype(jnp.float32)
        for o in range(1, outer):
            value += far[pl.ds(pl.multiple_of(o * rows + at, 16), 16), :].astype(jnp.float32)
        served[pl.ds(at, 16), :] = value.astype(jnp.bfloat16)
        return carry

    lax.fori_loop(0, rows // 16, total, 0)

    for copy in sends:
        copy.wait_send()

    def end_up(j, carry):
        mine, here, remote = up_copy(j)
        pl.when(jnp.logical_not(mine))(remote.wait_send)
        return carry

    lax.fori_loop(0, nseg, end_up, 0)
    for sg in range(groups):
        def end(sg=sg):
            for d in range(groups):
                whole = up_group(lax.rem(g + groups - d, groups), sg)
                for c in range(1, cores):
                    rdma(whole, whole, tu_send.at[sg, d, c], tu_recv.at[sg, d],
                         to("tp", t, cores, c)).wait_send()

        pl.when(owner(sg) == t)(end)
    put_up.wait()
    put_down.wait()


def body(tokens, norm_gain, up_weight, down_weight):
    groups, shards, cores = (lax.axis_size(a) for a in ("gr", "fs", "tp"))
    segment = down_weight.shape[0]
    up = (norm_gain[:, None] * up_weight).astype(jnp.bfloat16)
    down = down_weight.astype(jnp.bfloat16)
    values = tokens.astype(jnp.float32)
    normed = (values * lax.rsqrt(jnp.mean(values * values, axis=1, keepdims=True) + 1e-06)).astype(
        jnp.bfloat16
    )
    rows, depth = tokens.shape
    inner = inner_size(shards)
    nseg = up.shape[1] // segment
    width = groups * segment
    bf = jnp.bfloat16
    dma = pltpu.SemaphoreType.DMA
    vmem = pl.BlockSpec(memory_space=pltpu.VMEM)
    hbm = pl.BlockSpec(memory_space=pl.ANY)
    return pl.pallas_call(
        functools.partial(kernel, (groups, shards, cores)),
        out_shape=(
            jax.ShapeDtypeStruct((rows, depth), bf),
            jax.ShapeDtypeStruct((depth, width), bf),
            jax.ShapeDtypeStruct((width, depth), bf),
        ),
        in_specs=[vmem] * 3,
        out_specs=(vmem, hbm, hbm),
        scratch_shapes=[
            pltpu.VMEM((shards * rows, depth), bf),
            pltpu.VMEM((depth, width), bf),
            pltpu.VMEM((width, depth), bf),
            pltpu.VMEM((inner * rows, width), bf),
            pltpu.VMEM((shards * rows, depth), bf),
            pltpu.VMEM((shards * rows, depth), bf),
            pltpu.VMEM((shards // inner * rows, depth), bf),
            dma((nseg,)), dma((groups, shards)),
            dma((groups, groups, shards)), dma((groups, groups, shards)),
            dma((groups, groups, cores)), dma((groups, groups)),
            dma((groups,)), dma((groups,)),
            dma((cores, groups)), dma((cores, groups)),
            dma((shards,)), dma((shards,)),
            dma((shards,)), dma((shards,)),
            dma((shards // inner,)), dma((shards // inner,)),
            dma((2,)), dma((2,)),
        ],
        compiler_params=pltpu.CompilerParams(
            collective_id=0, has_side_effects=True, vmem_limit_bytes=48 * 1024 * 1024
        ),
        name="serve",
    )(normed, up, down)


def solution(mesh):
    return jax.shard_map(
        body,
        mesh=mesh,
        in_specs=(
            P(("gr", "fs", "tp"), None),
            P(("gr", "fs")),
            P(("gr", "fs"), "tp"),
            P(("gr", "fs"), "tp"),
        ),
        out_specs=(P(("gr", "fs", "tp"), None), P(None, "fs"), P("fs", None)),
        check_vma=False,
    )
```

```python
import functools

import jax
import jax.numpy as jnp
from jax import lax
from jax.experimental import pallas as pl
from jax.experimental.pallas import tpu as pltpu
from jax.sharding import PartitionSpec as P

MESH = pl.DeviceIdType.MESH
TILE = 256


def inner_size(shards):
    return max(d for d in range(1, shards + 1) if shards % d == 0 and d * d <= shards)


def kernel(sizes, normed, up, down, served, out_up, out_down, tok, su, sd, hid, part, got, far, *sems):
    groups, shards, cores = sizes
    inner = inner_size(shards)
    outer = shards // inner
    (up_send, up_recv, gu_send, gu_recv, tu_send, tu_recv, gd_send, gd_recv,
     td_send, td_recv, tok_send, tok_recv, part_send, part_recv, far_send, far_recv, hop_send, local, out_sem) = sems
    g, f, t = lax.axis_index("gr"), lax.axis_index("fs"), lax.axis_index("tp")
    z, y = f // inner, lax.rem(f, inner)
    rows, depth = normed.shape
    own_rows = up.shape[0]
    segment, dcols = down.shape
    nseg = up.shape[1] // segment
    group_rows = shards * own_rows

    def to(axis, me, size, step):
        return {axis: lax.rem(me + step, size)}

    def rdma(src, dst, send, recv, device):
        return pltpu.make_async_remote_copy(
            src_ref=src, dst_ref=dst, send_sem=send, recv_sem=recv,
            device_id=device, device_id_type=MESH,
        )

    def back(o, i):
        return {"fs": lax.rem(z + outer - o, outer) * inner + lax.rem(y + inner - i, inner)}

    def ahead(o, i):
        return {"fs": lax.rem(z + o, outer) * inner + lax.rem(y + i, inner)}

    def block_of(ref, number, count=1):
        return ref.at[pl.ds(pl.multiple_of(number * rows, rows), count * rows)]

    peers = [to("fs", f, shards, k) for k in range(1, shards)]
    peers += [to("gr", g, groups, k) for k in range(1, groups)]
    peers += [to("tp", t, cores, k) for k in range(1, cores)]
    barrier = pltpu.get_barrier_semaphore()
    for peer in peers:
        pl.semaphore_signal(barrier, inc=1, device_id=peer, device_id_type=MESH)
    pl.semaphore_wait(barrier, len(peers))

    def up_block(group, shard, sg):
        row = pl.multiple_of((group * shards + shard) * own_rows, own_rows)
        return su.at[pl.ds(row, own_rows), pl.ds(pl.multiple_of(sg * segment, segment), segment)]

    def up_group(group, sg):
        row = pl.multiple_of(group * group_rows, group_rows)
        return su.at[pl.ds(row, group_rows), pl.ds(sg * segment, segment)]

    def down_block(group, core):
        row = pl.multiple_of(group * segment, segment)
        return sd.at[pl.ds(row, segment), pl.ds(pl.multiple_of(core * dcols, dcols), dcols)]

    def owner(sg):
        return (sg * shards + f) // nseg

    def up_copy(i):
        number = t * nseg + i
        shard, sg = lax.rem(number, shards), number // shards
        step = lax.rem(shard - f + shards, shards)
        src = up.at[:, pl.ds(pl.multiple_of(i * segment, segment), segment)]
        remote = rdma(src, up_block(g, f, sg), up_send.at[i], up_recv.at[sg, step], {"fs": shard})
        here = pltpu.make_async_copy(src, up_block(g, f, sg), up_recv.at[sg, 0])
        return shard == f, here, remote

    def start_up(j, carry):
        mine, here, remote = up_copy(lax.rem(f + j, nseg))
        pl.when(mine)(here.start)
        pl.when(jnp.logical_not(mine))(remote.start)
        return carry

    lax.fori_loop(0, nseg, start_up, 0)

    sends = []
    keep_down = pltpu.make_async_copy(down, down_block(g, t), local.at[0])
    keep_tok = pltpu.make_async_copy(normed, block_of(tok, 0), local.at[1])
    keep_down.start()
    keep_tok.start()
    down_in = []
    for k in range(1, groups):
        copy = rdma(down, down_block(g, t), gd_send.at[k], gd_recv.at[k], to("gr", g, groups, k))
        copy.start()
        sends.append(copy)
        source = lax.rem(g + groups - k, groups)
        down_in.append((k, source))
    for k in range(1, cores):
        copy = rdma(down, down_block(g, t), td_send.at[k, 0], td_recv.at[k, 0], to("tp", t, cores, k))
        copy.start()
        sends.append(copy)

    for i in range(1, inner):
        copy = rdma(normed, block_of(tok, i), tok_send.at[i], tok_recv.at[i], ahead(0, i))
        copy.start()
        sends.append(copy)

    def beside(step):
        return {"fs": (z + step) * inner + y}

    def hop(o, step):
        source = normed if o in (0, outer) else block_of(tok, o * inner)
        n = (o + step) * inner
        return rdma(source, block_of(tok, n), hop_send.at[o + step if step > 0 else outer + o + step], tok_recv.at[n], beside(step))

    low, high = z > 0, z < outer - 1
    hops = []

    def move(o, step, when):
        pl.when(when)(lambda: hop(o, step).start())
        hops.append((o, step, when))

    move(0, 1, high)
    move(outer, -1, low)

    for sg in range(groups):
        def forward(sg=sg):
            def arrived(k, carry):
                shard = lax.rem(f + shards - k, shards)
                block = up_block(g, shard, sg)

                @pl.when(k == 0)
                def _():
                    pltpu.make_async_copy(block, block, up_recv.at[sg, 0]).wait()

                @pl.when(k > 0)
                def _():
                    rdma(block, block, up_send.at[0], up_recv.at[sg, k], {"fs": shard}).wait_recv()

                for d in range(1, groups):
                    rdma(block, block, gu_send.at[sg, d, k], gu_recv.at[sg, d, k],
                         to("gr", g, groups, d)).start()
                return carry

            lax.fori_loop(0, shards, arrived, 0)
            whole = up_group(g, sg)
            for c in range(1, cores):
                rdma(whole, whole, tu_send.at[sg, 0, c], tu_recv.at[sg, 0], to("tp", t, cores, c)).start()

        pl.when(owner(sg) == t)(forward)

    for o in range(1, outer):
        for n, when, step, more in ((o, z >= o, 1, high), (outer - o, z + o < outer, -1, low)):
            block = block_of(tok, n * inner)

            @pl.when(when)
            def _(n=n, step=step, block=block):
                rdma(block, block, tok_send.at[0], tok_recv.at[n * inner], beside(-step)).wait_recv()

            if 0 < n + step < outer:
                move(n, step, when & more)

            @pl.when(when)
            def _(n=n, block=block):
                for i in range(1, inner):
                    at = n * inner + i
                    rdma(block, block_of(tok, at), tok_send.at[at], tok_recv.at[at], ahead(0, i)).start()

    for k, source in down_in:
        block = down_block(source, t)
        rdma(block, block, gd_send.at[k], gd_recv.at[k], {"gr": source}).wait_recv()
        for c in range(1, cores):
            copy = rdma(block, block, td_send.at[c, k], td_recv.at[c, k], to("tp", t, cores, c))
            copy.start()
            sends.append(copy)

    for sg in range(groups):
        def onward(sg=sg):
            for d in range(1, groups):
                source = lax.rem(g + groups - d, groups)

                def arrived(k, carry):
                    block = up_block(source, lax.rem(f + shards - k, shards), sg)
                    rdma(block, block, gu_send.at[sg, d, k], gu_recv.at[sg, d, k], {"gr": source}).wait()
                    return carry

                lax.fori_loop(0, shards, arrived, 0)
                whole = up_group(source, sg)
                for c in range(1, cores):
                    rdma(whole, whole, tu_send.at[sg, d, c], tu_recv.at[sg, d],
                         to("tp", t, cores, c)).start()

        pl.when(owner(sg) == t)(onward)

    keep_down.wait()
    keep_tok.wait()
    for c in range(1, cores):
        core = lax.rem(t + cores - c, cores)
        for k in range(groups):
            block = down_block(lax.rem(g + groups - k, groups), core)
            rdma(block, block, td_send.at[c, k], td_recv.at[c, k], {"tp": core}).wait_recv()
    for sg in range(groups):
        def take(sg=sg):
            for d in range(groups):
                whole = up_group(lax.rem(g + groups - d, groups), sg)
                rdma(whole, whole, tu_send.at[sg, d, 1], tu_recv.at[sg, d],
                     {"tp": owner(sg)}).wait_recv()

        pl.when(owner(sg) != t)(take)

    put_up = pltpu.make_async_copy(su, out_up, out_sem.at[0])
    put_down = pltpu.make_async_copy(sd, out_down, out_sem.at[1])
    put_up.start()
    put_down.start()

    width = su.shape[1]
    stack = inner * rows

    def near_copy(o, i):
        n = o * inner + i
        return rdma(block_of(part, n), block_of(got, n), part_send.at[n], part_recv.at[n], back(0, i))

    def far_copy(o):
        right = o > z
        step = jnp.where(right, 1, -1)
        last = jnp.where(right, o == outer - 1, o == 1)
        slot = jnp.where(last, jnp.where(right, 0, outer), o + step)
        return rdma(block_of(part, o * inner), block_of(far, slot), far_send.at[o], far_recv.at[slot],
                    beside(step))

    def far_arrived(slot, step):
        rdma(block_of(far, slot), block_of(far, slot), far_send.at[0], far_recv.at[slot],
             beside(step)).wait_recv()

    def compute(o):
        for i in range(1, inner):
            block = block_of(tok, o * inner + i)
            n = o * inner + i
            rdma(block, block, tok_send.at[n], tok_recv.at[n], back(0, i)).wait_recv()
        both = pl.ds(pl.multiple_of(o * stack, stack), stack)

        def first(n, carry):
            cols = pl.ds(pl.multiple_of(n * TILE, TILE), TILE)
            product = jnp.dot(tok[both, :], su[:, cols], preferred_element_type=jnp.float32)
            product = jnp.maximum(product, 0.0)
            hid[:, cols] = (product * product).astype(jnp.bfloat16)
            return carry

        lax.fori_loop(0, width // TILE, first, 0)

        def second(n, carry):
            cols = pl.ds(pl.multiple_of(n * TILE, TILE), TILE)
            product = jnp.dot(hid[...], sd[:, cols], preferred_element_type=jnp.float32)
            part[both, cols] = product.astype(jnp.bfloat16)
            return carry

        lax.fori_loop(0, depth // TILE, second, 0)
        for i in range(1, inner):
            near_copy(o, i).start()

    def gather(o):
        for i in range(1, inner):
            near_copy(o, i).wait()

    def add(o):
        gather(o)

        def sum_up(passed):
            def chunk(r, carry):
                at = pl.multiple_of(r * 16, 16)
                mine = pl.ds(pl.multiple_of(o * stack + at, 16), 16)
                value = part[mine, :].astype(jnp.float32)
                for i in range(1, inner):
                    near = pl.ds(pl.multiple_of(o * stack + i * rows + at, 16), 16)
                    value += got[near, :].astype(jnp.float32)
                if passed:
                    value += far[pl.ds(pl.multiple_of(o * rows + at, 16), 16), :].astype(jnp.float32)
                part[mine, :] = value.astype(jnp.bfloat16)
                return carry

            lax.fori_loop(0, rows // 16, chunk, 0)

        right = o > z
        passed = (right & low) | (jnp.logical_not(right) & high)

        @pl.when(passed)
        def _():
            far_arrived(o, jnp.where(right, -1, 1))
            sum_up(True)

        pl.when(jnp.logical_not(passed))(lambda: sum_up(False))
        far_copy(o).start()

    order = []
    left_end, right_end = z * 0, z * 0 + outer - 1
    for _ in range(outer):
        take_left = z - left_end > right_end - z
        owner_z = jnp.where(take_left, left_end, right_end)
        order.append(lax.rem(z - owner_z + outer, outer))
        left_end = jnp.where(take_left, left_end + 1, left_end)
        right_end = jnp.where(take_left, right_end, right_end - 1)

    for o in order:
        compute(o)
    for o in order[:-1]:
        add(o)
    gather(0)
    pl.when(low)(lambda: far_arrived(0, -1))
    pl.when(high)(lambda: far_arrived(outer, 1))

    def total(ends):
        def chunk(r, carry):
            at = pl.multiple_of(r * 16, 16)
            value = part[pl.ds(at, 16), :].astype(jnp.float32)
            for i in range(1, inner):
                value += got[pl.ds(pl.multiple_of(i * rows + at, 16), 16), :].astype(jnp.float32)
            for end in ends:
                value += far[pl.ds(pl.multiple_of(end * rows + at, 16), 16), :].astype(jnp.float32)
            served[pl.ds(at, 16), :] = value.astype(jnp.bfloat16)
            return carry

        lax.fori_loop(0, rows // 16, chunk, 0)

    pl.when(low & high)(lambda: total((0, outer)))
    pl.when(low & jnp.logical_not(high))(lambda: total((0,)))
    pl.when(jnp.logical_not(low) & high)(lambda: total((outer,)))
    pl.when(jnp.logical_not(low | high))(lambda: total(()))

    for o, step, when in hops:
        pl.when(when)(lambda o=o, step=step: hop(o, step).wait_send())
    for n in range(inner, shards):
        if n % inner:
            block = block_of(tok, n)
            rdma(block, block, tok_send.at[n], tok_recv.at[n], ahead(0, n % inner)).wait_send()
    for o in range(1, outer):
        far_copy(o).wait_send()
    for copy in sends:
        copy.wait_send()

    def end_up(j, carry):
        mine, here, remote = up_copy(j)
        pl.when(jnp.logical_not(mine))(remote.wait_send)
        return carry

    lax.fori_loop(0, nseg, end_up, 0)
    for sg in range(groups):
        def end(sg=sg):
            for d in range(groups):
                whole = up_group(lax.rem(g + groups - d, groups), sg)
                for c in range(1, cores):
                    rdma(whole, whole, tu_send.at[sg, d, c], tu_recv.at[sg, d],
                         to("tp", t, cores, c)).wait_send()

        pl.when(owner(sg) == t)(end)
    put_up.wait()
    put_down.wait()


def body(tokens, norm_gain, up_weight, down_weight):
    groups, shards, cores = (lax.axis_size(a) for a in ("gr", "fs", "tp"))
    segment = down_weight.shape[0]
    up = (norm_gain[:, None] * up_weight).astype(jnp.bfloat16)
    down = down_weight.astype(jnp.bfloat16)
    values = tokens.astype(jnp.float32)
    normed = (values * lax.rsqrt(jnp.mean(values * values, axis=1, keepdims=True) + 1e-06)).astype(
        jnp.bfloat16
    )
    rows, depth = tokens.shape
    inner = inner_size(shards)
    nseg = up.shape[1] // segment
    width = groups * segment
    bf = jnp.bfloat16
    dma = pltpu.SemaphoreType.DMA
    vmem = pl.BlockSpec(memory_space=pltpu.VMEM)
    hbm = pl.BlockSpec(memory_space=pl.ANY)
    return pl.pallas_call(
        functools.partial(kernel, (groups, shards, cores)),
        out_shape=(
            jax.ShapeDtypeStruct((rows, depth), bf),
            jax.ShapeDtypeStruct((depth, width), bf),
            jax.ShapeDtypeStruct((width, depth), bf),
        ),
        in_specs=[vmem] * 3,
        out_specs=(vmem, hbm, hbm),
        scratch_shapes=[
            pltpu.VMEM((shards * rows, depth), bf),
            pltpu.VMEM((depth, width), bf),
            pltpu.VMEM((width, depth), bf),
            pltpu.VMEM((inner * rows, width), bf),
            pltpu.VMEM((shards * rows, depth), bf),
            pltpu.VMEM((shards * rows, depth), bf),
            pltpu.VMEM(((shards // inner + 1) * rows, depth), bf),
            dma((nseg,)), dma((groups, shards)),
            dma((groups, groups, shards)), dma((groups, groups, shards)),
            dma((groups, groups, cores)), dma((groups, groups)),
            dma((groups,)), dma((groups,)),
            dma((cores, groups)), dma((cores, groups)),
            dma((shards,)), dma((shards,)),
            dma((shards,)), dma((shards,)),
            dma((shards // inner,)), dma((shards // inner + 1,)), dma((2 * (shards // inner),)),
            dma((2,)), dma((2,)),
        ],
        compiler_params=pltpu.CompilerParams(
            collective_id=0, has_side_effects=True, vmem_limit_bytes=48 * 1024 * 1024
        ),
        name="serve",
    )(normed, up, down)


def solution(mesh):
    return jax.shard_map(
        body,
        mesh=mesh,
        in_specs=(
            P(("gr", "fs", "tp"), None),
            P(("gr", "fs")),
            P(("gr", "fs"), "tp"),
            P(("gr", "fs"), "tp"),
        ),
        out_specs=(P(("gr", "fs", "tp"), None), P(None, "fs"), P("fs", None)),
        check_vma=False,
    )
```

```python
import functools

import jax
import jax.numpy as jnp
from jax import lax
from jax.experimental import pallas as pl
from jax.experimental.pallas import tpu as pltpu
from jax.sharding import PartitionSpec as P

MESH = pl.DeviceIdType.MESH
TILE = 256


def inner_size(shards):
    return max(d for d in range(1, shards + 1) if shards % d == 0 and d * d <= shards)


def kernel(sizes, normed, up, down, served, out_up, out_down, tok, su, sd, hid, part, got, far, *sems):
    groups, shards, cores = sizes
    inner = inner_size(shards)
    outer = shards // inner
    (up_send, up_recv, gu_send, gu_recv, tu_send, tu_recv, gd_send, gd_recv,
     td_send, td_recv, tok_send, tok_recv, part_send, part_recv, far_send, far_recv, hop_send, ou_send, ou_recv, local, out_sem) = sems
    g, f, t = lax.axis_index("gr"), lax.axis_index("fs"), lax.axis_index("tp")
    z, y = f // inner, lax.rem(f, inner)
    rows, depth = normed.shape
    own_rows = up.shape[0]
    segment, dcols = down.shape
    nseg = up.shape[1] // segment
    group_rows = shards * own_rows

    def to(axis, me, size, step):
        return {axis: lax.rem(me + step, size)}

    def rdma(src, dst, send, recv, device):
        return pltpu.make_async_remote_copy(
            src_ref=src, dst_ref=dst, send_sem=send, recv_sem=recv,
            device_id=device, device_id_type=MESH,
        )

    def back(o, i):
        return {"fs": lax.rem(z + outer - o, outer) * inner + lax.rem(y + inner - i, inner)}

    def ahead(o, i):
        return {"fs": lax.rem(z + o, outer) * inner + lax.rem(y + i, inner)}

    def block_of(ref, number, count=1):
        return ref.at[pl.ds(pl.multiple_of(number * rows, rows), count * rows)]

    peers = [to("fs", f, shards, k) for k in range(1, shards)]
    peers += [to("gr", g, groups, k) for k in range(1, groups)]
    peers += [to("tp", t, cores, k) for k in range(1, cores)]
    barrier = pltpu.get_barrier_semaphore()
    for peer in peers:
        pl.semaphore_signal(barrier, inc=1, device_id=peer, device_id_type=MESH)
    pl.semaphore_wait(barrier, len(peers))

    def up_block(group, shard, sg):
        row = pl.multiple_of((group * shards + shard) * own_rows, own_rows)
        return su.at[pl.ds(row, own_rows), pl.ds(pl.multiple_of(sg * segment, segment), segment)]

    def up_group(group, sg):
        row = pl.multiple_of(group * group_rows, group_rows)
        return su.at[pl.ds(row, group_rows), pl.ds(sg * segment, segment)]

    def down_block(group, core):
        row = pl.multiple_of(group * segment, segment)
        return sd.at[pl.ds(row, segment), pl.ds(pl.multiple_of(core * dcols, dcols), dcols)]

    def owner(sg):
        return (sg * shards + f) // nseg

    sends = []
    keep_down = pltpu.make_async_copy(down, down_block(g, t), local.at[0])
    keep_tok = pltpu.make_async_copy(normed, block_of(tok, 0), local.at[1])
    keep_down.start()
    keep_tok.start()
    down_in = []
    for k in range(1, groups):
        copy = rdma(down, down_block(g, t), gd_send.at[k], gd_recv.at[k], to("gr", g, groups, k))
        copy.start()
        sends.append(copy)
        source = lax.rem(g + groups - k, groups)
        down_in.append((k, source))
    for k in range(1, cores):
        copy = rdma(down, down_block(g, t), td_send.at[k, 0], td_recv.at[k, 0], to("tp", t, cores, k))
        copy.start()
        sends.append(copy)

    for i in range(1, inner):
        copy = rdma(normed, block_of(tok, i), tok_send.at[i], tok_recv.at[i], ahead(0, i))
        copy.start()
        sends.append(copy)

    def beside(step):
        return {"fs": (z + step) * inner + y}

    def hop(o, step):
        source = normed if o in (0, outer) else block_of(tok, o * inner)
        n = (o + step) * inner
        return rdma(source, block_of(tok, n), hop_send.at[o + step if step > 0 else outer + o + step], tok_recv.at[n], beside(step))

    low, high = z > 0, z < outer - 1
    hops = []

    def move(o, step, when):
        pl.when(when)(lambda: hop(o, step).start())
        hops.append((o, step, when))

    move(0, 1, high)
    move(outer, -1, low)

    def up_copy(i):
        number = t * nseg + i
        shard, sg = lax.rem(number, shards), number // shards
        step = lax.rem(shard - f + shards, shards)
        src = up.at[:, pl.ds(pl.multiple_of(i * segment, segment), segment)]
        remote = rdma(src, up_block(g, f, sg), up_send.at[i], up_recv.at[sg, step], {"fs": shard})
        here = pltpu.make_async_copy(src, up_block(g, f, sg), up_recv.at[sg, 0])
        return shard == f, here, remote

    def start_up(j, carry):
        mine, here, remote = up_copy(lax.rem(f + j, nseg))
        pl.when(mine)(here.start)
        pl.when(jnp.logical_not(mine))(remote.start)
        return carry

    lax.fori_loop(0, nseg, start_up, 0)

    def pass_on(o):
        for n, when, step, more in ((o, z >= o, 1, high), (outer - o, z + o < outer, -1, low)):
            block = block_of(tok, n * inner)

            @pl.when(when)
            def _(n=n, step=step, block=block):
                rdma(block, block, tok_send.at[0], tok_recv.at[n * inner], beside(-step)).wait_recv()

            if 0 < n + step < outer:
                move(n, step, when & more)

            @pl.when(when)
            def _(n=n, block=block):
                for i in range(1, inner):
                    at = n * inner + i
                    rdma(block, block_of(tok, at), tok_send.at[at], tok_recv.at[at], ahead(0, i)).start()

    if outer > 1:
        pass_on(1)

    for sg in range(groups):
        def forward(sg=sg):
            def arrived(k, carry):
                shard = lax.rem(f + shards - k, shards)
                block = up_block(g, shard, sg)

                @pl.when(k == 0)
                def _():
                    pltpu.make_async_copy(block, block, up_recv.at[sg, 0]).wait()

                @pl.when(k > 0)
                def _():
                    rdma(block, block, up_send.at[0], up_recv.at[sg, k], {"fs": shard}).wait_recv()

                for d in range(1, groups):
                    rdma(block, block, gu_send.at[sg, d, k], gu_recv.at[sg, d, k],
                         to("gr", g, groups, d)).start()
                return carry

            lax.fori_loop(0, shards, arrived, 0)
            whole = up_group(g, sg)
            for c in range(1, cores):
                rdma(whole, whole, tu_send.at[sg, 0, c], tu_recv.at[sg, 0], to("tp", t, cores, c)).start()

        pl.when(owner(sg) == t)(forward)

    for o in range(2, outer):
        pass_on(o)

    for k, source in down_in:
        block = down_block(source, t)
        rdma(block, block, gd_send.at[k], gd_recv.at[k], {"gr": source}).wait_recv()
        for c in range(1, cores):
            copy = rdma(block, block, td_send.at[c, k], td_recv.at[c, k], to("tp", t, cores, c))
            copy.start()
            sends.append(copy)

    for sg in range(groups):
        def onward(sg=sg):
            for d in range(1, groups):
                source = lax.rem(g + groups - d, groups)

                def arrived(k, carry):
                    block = up_block(source, lax.rem(f + shards - k, shards), sg)
                    rdma(block, block, gu_send.at[sg, d, k], gu_recv.at[sg, d, k], {"gr": source}).wait()
                    for c in range(1, cores):
                        rdma(block, block, ou_send.at[sg, d, c, k], ou_recv.at[sg, d, k],
                             to("tp", t, cores, c)).start()
                    return carry

                lax.fori_loop(0, shards, arrived, 0)

        pl.when(owner(sg) == t)(onward)

    keep_down.wait()
    keep_tok.wait()
    for c in range(1, cores):
        core = lax.rem(t + cores - c, cores)
        for k in range(groups):
            block = down_block(lax.rem(g + groups - k, groups), core)
            rdma(block, block, td_send.at[c, k], td_recv.at[c, k], {"tp": core}).wait_recv()
    for sg in range(groups):
        def take(sg=sg):
            whole = up_group(g, sg)
            rdma(whole, whole, tu_send.at[sg, 0, 1], tu_recv.at[sg, 0], {"tp": owner(sg)}).wait_recv()
            for d in range(1, groups):
                def taken(k, carry):
                    block = up_block(lax.rem(g + groups - d, groups), lax.rem(f + shards - k, shards), sg)
                    rdma(block, block, tu_send.at[sg, 0, 1], ou_recv.at[sg, d, k],
                         {"tp": owner(sg)}).wait_recv()
                    return carry

                lax.fori_loop(0, shards, taken, 0)

        pl.when(owner(sg) != t)(take)

    put_up = pltpu.make_async_copy(su, out_up, out_sem.at[0])
    put_down = pltpu.make_async_copy(sd, out_down, out_sem.at[1])
    put_up.start()
    put_down.start()

    width = su.shape[1]
    stack = inner * rows

    def near_copy(o, i):
        n = o * inner + i
        return rdma(block_of(part, n), block_of(got, n), part_send.at[n], part_recv.at[n], back(0, i))

    def far_copy(o):
        right = o > z
        step = jnp.where(right, 1, -1)
        last = jnp.where(right, o == outer - 1, o == 1)
        slot = jnp.where(last, jnp.where(right, 0, outer), o + step)
        return rdma(block_of(part, o * inner), block_of(far, slot), far_send.at[o], far_recv.at[slot],
                    beside(step))

    def far_arrived(slot, step):
        rdma(block_of(far, slot), block_of(far, slot), far_send.at[0], far_recv.at[slot],
             beside(step)).wait_recv()

    def compute(o):
        for i in range(1, inner):
            block = block_of(tok, o * inner + i)
            n = o * inner + i
            rdma(block, block, tok_send.at[n], tok_recv.at[n], back(0, i)).wait_recv()
        both = pl.ds(pl.multiple_of(o * stack, stack), stack)

        def first(n, carry):
            cols = pl.ds(pl.multiple_of(n * TILE, TILE), TILE)
            product = jnp.dot(tok[both, :], su[:, cols], preferred_element_type=jnp.float32)
            product = jnp.maximum(product, 0.0)
            hid[:, cols] = (product * product).astype(jnp.bfloat16)
            return carry

        lax.fori_loop(0, width // TILE, first, 0)

        def second(n, carry):
            cols = pl.ds(pl.multiple_of(n * TILE, TILE), TILE)
            product = jnp.dot(hid[...], sd[:, cols], preferred_element_type=jnp.float32)
            part[both, cols] = product.astype(jnp.bfloat16)
            return carry

        lax.fori_loop(0, depth // TILE, second, 0)
        for i in range(1, inner):
            near_copy(o, i).start()

    def gather(o):
        for i in range(1, inner):
            near_copy(o, i).wait()

    def add(o):
        gather(o)

        def sum_up(passed):
            def chunk(r, carry):
                at = pl.multiple_of(r * 16, 16)
                mine = pl.ds(pl.multiple_of(o * stack + at, 16), 16)
                value = part[mine, :].astype(jnp.float32)
                for i in range(1, inner):
                    near = pl.ds(pl.multiple_of(o * stack + i * rows + at, 16), 16)
                    value += got[near, :].astype(jnp.float32)
                if passed:
                    value += far[pl.ds(pl.multiple_of(o * rows + at, 16), 16), :].astype(jnp.float32)
                part[mine, :] = value.astype(jnp.bfloat16)
                return carry

            lax.fori_loop(0, rows // 16, chunk, 0)

        right = o > z
        passed = (right & low) | (jnp.logical_not(right) & high)

        @pl.when(passed)
        def _():
            far_arrived(o, jnp.where(right, -1, 1))
            sum_up(True)

        pl.when(jnp.logical_not(passed))(lambda: sum_up(False))
        far_copy(o).start()

    order = []
    left_end, right_end = z * 0, z * 0 + outer - 1
    for _ in range(outer):
        take_left = z - left_end > right_end - z
        owner_z = jnp.where(take_left, left_end, right_end)
        order.append(lax.rem(z - owner_z + outer, outer))
        left_end = jnp.where(take_left, left_end + 1, left_end)
        right_end = jnp.where(take_left, right_end, right_end - 1)

    for o in order:
        compute(o)
    for o in order[:-1]:
        add(o)
    gather(0)
    pl.when(low)(lambda: far_arrived(0, -1))
    pl.when(high)(lambda: far_arrived(outer, 1))

    def total(ends):
        def chunk(r, carry):
            at = pl.multiple_of(r * 16, 16)
            value = part[pl.ds(at, 16), :].astype(jnp.float32)
            for i in range(1, inner):
                value += got[pl.ds(pl.multiple_of(i * rows + at, 16), 16), :].astype(jnp.float32)
            for end in ends:
                value += far[pl.ds(pl.multiple_of(end * rows + at, 16), 16), :].astype(jnp.float32)
            served[pl.ds(at, 16), :] = value.astype(jnp.bfloat16)
            return carry

        lax.fori_loop(0, rows // 16, chunk, 0)

    pl.when(low & high)(lambda: total((0, outer)))
    pl.when(low & jnp.logical_not(high))(lambda: total((0,)))
    pl.when(jnp.logical_not(low) & high)(lambda: total((outer,)))
    pl.when(jnp.logical_not(low | high))(lambda: total(()))

    for o, step, when in hops:
        pl.when(when)(lambda o=o, step=step: hop(o, step).wait_send())
    for n in range(inner, shards):
        if n % inner:
            block = block_of(tok, n)
            rdma(block, block, tok_send.at[n], tok_recv.at[n], ahead(0, n % inner)).wait_send()
    for o in range(1, outer):
        far_copy(o).wait_send()
    for copy in sends:
        copy.wait_send()

    def end_up(j, carry):
        mine, here, remote = up_copy(j)
        pl.when(jnp.logical_not(mine))(remote.wait_send)
        return carry

    lax.fori_loop(0, nseg, end_up, 0)
    for sg in range(groups):
        def end(sg=sg):
            whole = up_group(g, sg)
            for c in range(1, cores):
                rdma(whole, whole, tu_send.at[sg, 0, c], tu_recv.at[sg, 0],
                     to("tp", t, cores, c)).wait_send()
            for d in range(1, groups):
                def left(k, carry):
                    block = up_block(lax.rem(g + groups - d, groups), lax.rem(f + shards - k, shards), sg)
                    for c in range(1, cores):
                        rdma(block, block, ou_send.at[sg, d, c, k], ou_recv.at[sg, d, k],
                             to("tp", t, cores, c)).wait_send()
                    return carry

                lax.fori_loop(0, shards, left, 0)

        pl.when(owner(sg) == t)(end)
    put_up.wait()
    put_down.wait()


def body(tokens, norm_gain, up_weight, down_weight):
    groups, shards, cores = (lax.axis_size(a) for a in ("gr", "fs", "tp"))
    segment = down_weight.shape[0]
    up = (norm_gain[:, None] * up_weight).astype(jnp.bfloat16)
    down = down_weight.astype(jnp.bfloat16)
    values = tokens.astype(jnp.float32)
    normed = (values * lax.rsqrt(jnp.mean(values * values, axis=1, keepdims=True) + 1e-06)).astype(
        jnp.bfloat16
    )
    rows, depth = tokens.shape
    inner = inner_size(shards)
    nseg = up.shape[1] // segment
    width = groups * segment
    bf = jnp.bfloat16
    dma = pltpu.SemaphoreType.DMA
    vmem = pl.BlockSpec(memory_space=pltpu.VMEM)
    hbm = pl.BlockSpec(memory_space=pl.ANY)
    return pl.pallas_call(
        functools.partial(kernel, (groups, shards, cores)),
        out_shape=(
            jax.ShapeDtypeStruct((rows, depth), bf),
            jax.ShapeDtypeStruct((depth, width), bf),
            jax.ShapeDtypeStruct((width, depth), bf),
        ),
        in_specs=[vmem] * 3,
        out_specs=(vmem, hbm, hbm),
        scratch_shapes=[
            pltpu.VMEM((shards * rows, depth), bf),
            pltpu.VMEM((depth, width), bf),
            pltpu.VMEM((width, depth), bf),
            pltpu.VMEM((inner * rows, width), bf),
            pltpu.VMEM((shards * rows, depth), bf),
            pltpu.VMEM((shards * rows, depth), bf),
            pltpu.VMEM(((shards // inner + 1) * rows, depth), bf),
            dma((nseg,)), dma((groups, shards)),
            dma((groups, groups, shards)), dma((groups, groups, shards)),
            dma((groups, groups, cores)), dma((groups, groups)),
            dma((groups,)), dma((groups,)),
            dma((cores, groups)), dma((cores, groups)),
            dma((shards,)), dma((shards,)),
            dma((shards,)), dma((shards,)),
            dma((shards // inner,)), dma((shards // inner + 1,)), dma((2 * (shards // inner),)),
            dma((groups, groups, cores, shards)), dma((groups, groups, shards)),
            dma((2,)), dma((2,)),
        ],
        compiler_params=pltpu.CompilerParams(
            collective_id=0, has_side_effects=True, vmem_limit_bytes=48 * 1024 * 1024
        ),
        name="serve",
    )(normed, up, down)


def solution(mesh):
    return jax.shard_map(
        body,
        mesh=mesh,
        in_specs=(
            P(("gr", "fs", "tp"), None),
            P(("gr", "fs")),
            P(("gr", "fs"), "tp"),
            P(("gr", "fs"), "tp"),
        ),
        out_specs=(P(("gr", "fs", "tp"), None), P(None, "fs"), P("fs", None)),
        check_vma=False,
    )
```

```python
import functools

import jax
import jax.numpy as jnp
from jax import lax
from jax.experimental import pallas as pl
from jax.experimental.pallas import tpu as pltpu
from jax.sharding import PartitionSpec as P

MESH = pl.DeviceIdType.MESH
TILE = 256


def inner_size(shards):
    return max(d for d in range(1, shards + 1) if shards % d == 0 and d * d <= shards)


def kernel(sizes, normed, up, down, served, su, sd, tok, hid, part, got, far, *sems):
    groups, shards, cores = sizes
    inner = inner_size(shards)
    outer = shards // inner
    (up_send, up_recv, gu_send, gu_recv, tu_send, tu_recv, gd_send, gd_recv,
     td_send, td_recv, tok_send, tok_recv, part_send, part_recv, far_send, far_recv, hop_send, ou_send, ou_recv, local) = sems
    g, f, t = lax.axis_index("gr"), lax.axis_index("fs"), lax.axis_index("tp")
    z, y = f // inner, lax.rem(f, inner)
    rows, depth = normed.shape
    own_rows = up.shape[0]
    segment, dcols = down.shape
    nseg = up.shape[1] // segment
    group_rows = shards * own_rows

    def to(axis, me, size, step):
        return {axis: lax.rem(me + step, size)}

    def rdma(src, dst, send, recv, device):
        return pltpu.make_async_remote_copy(
            src_ref=src, dst_ref=dst, send_sem=send, recv_sem=recv,
            device_id=device, device_id_type=MESH,
        )

    def back(o, i):
        return {"fs": lax.rem(z + outer - o, outer) * inner + lax.rem(y + inner - i, inner)}

    def ahead(o, i):
        return {"fs": lax.rem(z + o, outer) * inner + lax.rem(y + i, inner)}

    def block_of(ref, number, count=1):
        return ref.at[pl.ds(pl.multiple_of(number * rows, rows), count * rows)]

    peers = [to("fs", f, shards, k) for k in range(1, shards)]
    peers += [to("gr", g, groups, k) for k in range(1, groups)]
    peers += [to("tp", t, cores, k) for k in range(1, cores)]
    barrier = pltpu.get_barrier_semaphore()
    for peer in peers:
        pl.semaphore_signal(barrier, inc=1, device_id=peer, device_id_type=MESH)
    pl.semaphore_wait(barrier, len(peers))

    def up_block(group, shard, sg):
        row = pl.multiple_of((group * shards + shard) * own_rows, own_rows)
        return su.at[pl.ds(row, own_rows), pl.ds(pl.multiple_of(sg * segment, segment), segment)]

    def up_group(group, sg):
        row = pl.multiple_of(group * group_rows, group_rows)
        return su.at[pl.ds(row, group_rows), pl.ds(sg * segment, segment)]

    def down_block(group, core):
        row = pl.multiple_of(group * segment, segment)
        return sd.at[pl.ds(row, segment), pl.ds(pl.multiple_of(core * dcols, dcols), dcols)]

    def owner(sg):
        return (sg * shards + f) // nseg

    sends = []
    keep_down = pltpu.make_async_copy(down, down_block(g, t), local.at[0])
    keep_tok = pltpu.make_async_copy(normed, block_of(tok, 0), local.at[1])
    keep_down.start()
    keep_tok.start()
    down_in = []
    for k in range(1, groups):
        copy = rdma(down, down_block(g, t), gd_send.at[k], gd_recv.at[k], to("gr", g, groups, k))
        copy.start()
        sends.append(copy)
        source = lax.rem(g + groups - k, groups)
        down_in.append((k, source))
    for k in range(1, cores):
        copy = rdma(down, down_block(g, t), td_send.at[k, 0], td_recv.at[k, 0], to("tp", t, cores, k))
        copy.start()
        sends.append(copy)

    for i in range(1, inner):
        copy = rdma(normed, block_of(tok, i), tok_send.at[i], tok_recv.at[i], ahead(0, i))
        copy.start()
        sends.append(copy)

    def beside(step):
        return {"fs": (z + step) * inner + y}

    def hop(o, step):
        source = normed if o in (0, outer) else block_of(tok, o * inner)
        n = (o + step) * inner
        return rdma(source, block_of(tok, n), hop_send.at[o + step if step > 0 else outer + o + step], tok_recv.at[n], beside(step))

    low, high = z > 0, z < outer - 1
    hops = []

    def move(o, step, when):
        pl.when(when)(lambda: hop(o, step).start())
        hops.append((o, step, when))

    move(0, 1, high)
    move(outer, -1, low)

    def up_copy(i):
        number = t * nseg + i
        shard, sg = lax.rem(number, shards), number // shards
        step = lax.rem(shard - f + shards, shards)
        src = up.at[:, pl.ds(pl.multiple_of(i * segment, segment), segment)]
        remote = rdma(src, up_block(g, f, sg), up_send.at[i], up_recv.at[sg, step], {"fs": shard})
        here = pltpu.make_async_copy(src, up_block(g, f, sg), up_recv.at[sg, 0])
        return shard == f, here, remote

    def start_up(j, carry):
        mine, here, remote = up_copy(lax.rem(f + j, nseg))
        pl.when(mine)(here.start)
        pl.when(jnp.logical_not(mine))(remote.start)
        return carry

    lax.fori_loop(0, nseg, start_up, 0)

    def pass_on(o):
        for n, when, step, more in ((o, z >= o, 1, high), (outer - o, z + o < outer, -1, low)):
            block = block_of(tok, n * inner)

            @pl.when(when)
            def _(n=n, step=step, block=block):
                rdma(block, block, tok_send.at[0], tok_recv.at[n * inner], beside(-step)).wait_recv()

            if 0 < n + step < outer:
                move(n, step, when & more)

            @pl.when(when)
            def _(n=n, block=block):
                for i in range(1, inner):
                    at = n * inner + i
                    rdma(block, block_of(tok, at), tok_send.at[at], tok_recv.at[at], ahead(0, i)).start()

    if outer > 1:
        pass_on(1)

    for sg in range(groups):
        def forward(sg=sg):
            def arrived(k, carry):
                shard = lax.rem(f + shards - k, shards)
                block = up_block(g, shard, sg)

                @pl.when(k == 0)
                def _():
                    pltpu.make_async_copy(block, block, up_recv.at[sg, 0]).wait()

                @pl.when(k > 0)
                def _():
                    rdma(block, block, up_send.at[0], up_recv.at[sg, k], {"fs": shard}).wait_recv()

                for d in range(1, groups):
                    rdma(block, block, gu_send.at[sg, d, k], gu_recv.at[sg, d, k],
                         to("gr", g, groups, d)).start()
                return carry

            lax.fori_loop(0, shards, arrived, 0)
            whole = up_group(g, sg)
            for c in range(1, cores):
                rdma(whole, whole, tu_send.at[sg, 0, c], tu_recv.at[sg, 0], to("tp", t, cores, c)).start()

        pl.when(owner(sg) == t)(forward)

    for o in range(2, outer):
        pass_on(o)

    for k, source in down_in:
        block = down_block(source, t)
        rdma(block, block, gd_send.at[k], gd_recv.at[k], {"gr": source}).wait_recv()
        for c in range(1, cores):
            copy = rdma(block, block, td_send.at[c, k], td_recv.at[c, k], to("tp", t, cores, c))
            copy.start()
            sends.append(copy)

    for sg in range(groups):
        def onward(sg=sg):
            for d in range(1, groups):
                source = lax.rem(g + groups - d, groups)

                def arrived(k, carry):
                    block = up_block(source, lax.rem(f + shards - k, shards), sg)
                    rdma(block, block, gu_send.at[sg, d, k], gu_recv.at[sg, d, k], {"gr": source}).wait()
                    for c in range(1, cores):
                        rdma(block, block, ou_send.at[sg, d, c, k], ou_recv.at[sg, d, k],
                             to("tp", t, cores, c)).start()
                    return carry

                lax.fori_loop(0, shards, arrived, 0)

        pl.when(owner(sg) == t)(onward)

    keep_down.wait()
    keep_tok.wait()
    for c in range(1, cores):
        core = lax.rem(t + cores - c, cores)
        for k in range(groups):
            block = down_block(lax.rem(g + groups - k, groups), core)
            rdma(block, block, td_send.at[c, k], td_recv.at[c, k], {"tp": core}).wait_recv()
    for sg in range(groups):
        def take(sg=sg):
            whole = up_group(g, sg)
            rdma(whole, whole, tu_send.at[sg, 0, 1], tu_recv.at[sg, 0], {"tp": owner(sg)}).wait_recv()
            for d in range(1, groups):
                def taken(k, carry):
                    block = up_block(lax.rem(g + groups - d, groups), lax.rem(f + shards - k, shards), sg)
                    rdma(block, block, tu_send.at[sg, 0, 1], ou_recv.at[sg, d, k],
                         {"tp": owner(sg)}).wait_recv()
                    return carry

                lax.fori_loop(0, shards, taken, 0)

        pl.when(owner(sg) != t)(take)

    width = su.shape[1]
    stack = inner * rows

    def near_copy(o, i):
        n = o * inner + i
        return rdma(block_of(part, n), block_of(got, n), part_send.at[n], part_recv.at[n], back(0, i))

    def far_copy(o):
        right = o > z
        step = jnp.where(right, 1, -1)
        last = jnp.where(right, o == outer - 1, o == 1)
        slot = jnp.where(last, jnp.where(right, 0, outer), o + step)
        return rdma(block_of(part, o * inner), block_of(far, slot), far_send.at[o], far_recv.at[slot],
                    beside(step))

    def far_arrived(slot, step):
        rdma(block_of(far, slot), block_of(far, slot), far_send.at[0], far_recv.at[slot],
             beside(step)).wait_recv()

    def compute(o):
        for i in range(1, inner):
            block = block_of(tok, o * inner + i)
            n = o * inner + i
            rdma(block, block, tok_send.at[n], tok_recv.at[n], back(0, i)).wait_recv()
        both = pl.ds(pl.multiple_of(o * stack, stack), stack)

        def first(n, carry):
            cols = pl.ds(pl.multiple_of(n * TILE, TILE), TILE)
            product = jnp.dot(tok[both, :], su[:, cols], preferred_element_type=jnp.float32)
            product = jnp.maximum(product, 0.0)
            hid[:, cols] = (product * product).astype(jnp.bfloat16)
            return carry

        lax.fori_loop(0, width // TILE, first, 0)

        def second(n, carry):
            cols = pl.ds(pl.multiple_of(n * TILE, TILE), TILE)
            product = jnp.dot(hid[...], sd[:, cols], preferred_element_type=jnp.float32)
            part[both, cols] = product.astype(jnp.bfloat16)
            return carry

        lax.fori_loop(0, depth // TILE, second, 0)
        for i in range(1, inner):
            near_copy(o, i).start()

    def gather(o):
        for i in range(1, inner):
            near_copy(o, i).wait()

    def add(o):
        gather(o)

        def sum_up(passed):
            def chunk(r, carry):
                at = pl.multiple_of(r * 16, 16)
                mine = pl.ds(pl.multiple_of(o * stack + at, 16), 16)
                value = part[mine, :].astype(jnp.float32)
                for i in range(1, inner):
                    near = pl.ds(pl.multiple_of(o * stack + i * rows + at, 16), 16)
                    value += got[near, :].astype(jnp.float32)
                if passed:
                    value += far[pl.ds(pl.multiple_of(o * rows + at, 16), 16), :].astype(jnp.float32)
                part[mine, :] = value.astype(jnp.bfloat16)
                return carry

            lax.fori_loop(0, rows // 16, chunk, 0)

        right = o > z
        passed = (right & low) | (jnp.logical_not(right) & high)

        @pl.when(passed)
        def _():
            far_arrived(o, jnp.where(right, -1, 1))
            sum_up(True)

        pl.when(jnp.logical_not(passed))(lambda: sum_up(False))
        far_copy(o).start()

    order = []
    left_end, right_end = z * 0, z * 0 + outer - 1
    for _ in range(outer):
        take_left = z - left_end > right_end - z
        owner_z = jnp.where(take_left, left_end, right_end)
        order.append(lax.rem(z - owner_z + outer, outer))
        left_end = jnp.where(take_left, left_end + 1, left_end)
        right_end = jnp.where(take_left, right_end, right_end - 1)

    for o in order:
        compute(o)
    for o in order[:-1]:
        add(o)
    gather(0)
    pl.when(low)(lambda: far_arrived(0, -1))
    pl.when(high)(lambda: far_arrived(outer, 1))

    def total(ends):
        def chunk(r, carry):
            at = pl.multiple_of(r * 16, 16)
            value = part[pl.ds(at, 16), :].astype(jnp.float32)
            for i in range(1, inner):
                value += got[pl.ds(pl.multiple_of(i * rows + at, 16), 16), :].astype(jnp.float32)
            for end in ends:
                value += far[pl.ds(pl.multiple_of(end * rows + at, 16), 16), :].astype(jnp.float32)
            served[pl.ds(at, 16), :] = value.astype(jnp.bfloat16)
            return carry

        lax.fori_loop(0, rows // 16, chunk, 0)

    pl.when(low & high)(lambda: total((0, outer)))
    pl.when(low & jnp.logical_not(high))(lambda: total((0,)))
    pl.when(jnp.logical_not(low) & high)(lambda: total((outer,)))
    pl.when(jnp.logical_not(low | high))(lambda: total(()))

    for o, step, when in hops:
        pl.when(when)(lambda o=o, step=step: hop(o, step).wait_send())
    for n in range(inner, shards):
        if n % inner:
            block = block_of(tok, n)
            rdma(block, block, tok_send.at[n], tok_recv.at[n], ahead(0, n % inner)).wait_send()
    for o in range(1, outer):
        far_copy(o).wait_send()
    for copy in sends:
        copy.wait_send()

    def end_up(j, carry):
        mine, here, remote = up_copy(j)
        pl.when(jnp.logical_not(mine))(remote.wait_send)
        return carry

    lax.fori_loop(0, nseg, end_up, 0)
    for sg in range(groups):
        def end(sg=sg):
            whole = up_group(g, sg)
            for c in range(1, cores):
                rdma(whole, whole, tu_send.at[sg, 0, c], tu_recv.at[sg, 0],
                     to("tp", t, cores, c)).wait_send()
            for d in range(1, groups):
                def left(k, carry):
                    block = up_block(lax.rem(g + groups - d, groups), lax.rem(f + shards - k, shards), sg)
                    for c in range(1, cores):
                        rdma(block, block, ou_send.at[sg, d, c, k], ou_recv.at[sg, d, k],
                             to("tp", t, cores, c)).wait_send()
                    return carry

                lax.fori_loop(0, shards, left, 0)

        pl.when(owner(sg) == t)(end)


def body(tokens, norm_gain, up_weight, down_weight):
    groups, shards, cores = (lax.axis_size(a) for a in ("gr", "fs", "tp"))
    segment = down_weight.shape[0]
    up = (norm_gain[:, None] * up_weight).astype(jnp.bfloat16)
    down = down_weight.astype(jnp.bfloat16)
    values = tokens.astype(jnp.float32)
    normed = (values * lax.rsqrt(jnp.mean(values * values, axis=1, keepdims=True) + 1e-06)).astype(
        jnp.bfloat16
    )
    rows, depth = tokens.shape
    inner = inner_size(shards)
    nseg = up.shape[1] // segment
    width = groups * segment
    bf = jnp.bfloat16
    dma = pltpu.SemaphoreType.DMA
    vmem = pl.BlockSpec(memory_space=pltpu.VMEM)
    return pl.pallas_call(
        functools.partial(kernel, (groups, shards, cores)),
        out_shape=(
            jax.ShapeDtypeStruct((rows, depth), bf),
            jax.ShapeDtypeStruct((depth, width), bf),
            jax.ShapeDtypeStruct((width, depth), bf),
        ),
        in_specs=[vmem] * 3,
        out_specs=(vmem, vmem, vmem),
        scratch_shapes=[
            pltpu.VMEM((shards * rows, depth), bf),
            pltpu.VMEM((inner * rows, width), bf),
            pltpu.VMEM((shards * rows, depth), bf),
            pltpu.VMEM((shards * rows, depth), bf),
            pltpu.VMEM(((shards // inner + 1) * rows, depth), bf),
            dma((nseg,)), dma((groups, shards)),
            dma((groups, groups, shards)), dma((groups, groups, shards)),
            dma((groups, groups, cores)), dma((groups, groups)),
            dma((groups,)), dma((groups,)),
            dma((cores, groups)), dma((cores, groups)),
            dma((shards,)), dma((shards,)),
            dma((shards,)), dma((shards,)),
            dma((shards // inner,)), dma((shards // inner + 1,)), dma((2 * (shards // inner),)),
            dma((groups, groups, cores, shards)), dma((groups, groups, shards)),
            dma((2,)),
        ],
        compiler_params=pltpu.CompilerParams(
            collective_id=0, has_side_effects=True, vmem_limit_bytes=34 * 1024 * 1024
        ),
        name="serve",
    )(normed, up, down)


def solution(mesh):
    return jax.shard_map(
        body,
        mesh=mesh,
        in_specs=(
            P(("gr", "fs", "tp"), None),
            P(("gr", "fs")),
            P(("gr", "fs"), "tp"),
            P(("gr", "fs"), "tp"),
        ),
        out_specs=(P(("gr", "fs", "tp"), None), P(None, "fs"), P("fs", None)),
        check_vma=False,
    )
```

```python
import functools

import jax
import jax.numpy as jnp
from jax import lax
from jax.experimental import pallas as pl
from jax.experimental.pallas import tpu as pltpu
from jax.sharding import PartitionSpec as P

MESH = pl.DeviceIdType.MESH
TILE = 512


def inner_size(shards):
    return max(d for d in range(1, shards + 1) if shards % d == 0 and d * d <= shards)


def kernel(sizes, normed, up, down, served, su, sd, tok, hid, part, got, far, *sems):
    groups, shards, cores = sizes
    inner = inner_size(shards)
    outer = shards // inner
    (up_send, up_recv, gu_send, gu_recv, tu_send, tu_recv, gd_send, gd_recv,
     td_send, td_recv, tok_send, tok_recv, part_send, part_recv, far_send, far_recv, hop_send, ou_send, ou_recv, local) = sems
    g, f, t = lax.axis_index("gr"), lax.axis_index("fs"), lax.axis_index("tp")
    z, y = f // inner, lax.rem(f, inner)
    rows, depth = normed.shape
    own_rows = up.shape[0]
    segment, dcols = down.shape
    nseg = up.shape[1] // segment
    group_rows = shards * own_rows

    def to(axis, me, size, step):
        return {axis: lax.rem(me + step, size)}

    def rdma(src, dst, send, recv, device):
        return pltpu.make_async_remote_copy(
            src_ref=src, dst_ref=dst, send_sem=send, recv_sem=recv,
            device_id=device, device_id_type=MESH,
        )

    def back(o, i):
        return {"fs": lax.rem(z + outer - o, outer) * inner + lax.rem(y + inner - i, inner)}

    def ahead(o, i):
        return {"fs": lax.rem(z + o, outer) * inner + lax.rem(y + i, inner)}

    def block_of(ref, number, count=1):
        return ref.at[pl.ds(pl.multiple_of(number * rows, rows), count * rows)]

    peers = [to("fs", f, shards, k) for k in range(1, shards)]
    peers += [to("gr", g, groups, k) for k in range(1, groups)]
    peers += [to("tp", t, cores, k) for k in range(1, cores)]
    barrier = pltpu.get_barrier_semaphore()
    for peer in peers:
        pl.semaphore_signal(barrier, inc=1, device_id=peer, device_id_type=MESH)
    pl.semaphore_wait(barrier, len(peers))

    def up_block(group, shard, sg):
        row = pl.multiple_of((group * shards + shard) * own_rows, own_rows)
        return su.at[pl.ds(row, own_rows), pl.ds(pl.multiple_of(sg * segment, segment), segment)]

    def up_group(group, sg):
        row = pl.multiple_of(group * group_rows, group_rows)
        return su.at[pl.ds(row, group_rows), pl.ds(sg * segment, segment)]

    def down_block(group, core):
        row = pl.multiple_of(group * segment, segment)
        return sd.at[pl.ds(row, segment), pl.ds(pl.multiple_of(core * dcols, dcols), dcols)]

    def owner(sg):
        return (sg * shards + f) // nseg

    sends = []
    keep_down = pltpu.make_async_copy(down, down_block(g, t), local.at[0])
    keep_tok = pltpu.make_async_copy(normed, block_of(tok, 0), local.at[1])
    keep_down.start()
    keep_tok.start()
    down_in = []
    for k in range(1, groups):
        copy = rdma(down, down_block(g, t), gd_send.at[k], gd_recv.at[k], to("gr", g, groups, k))
        copy.start()
        sends.append(copy)
        source = lax.rem(g + groups - k, groups)
        down_in.append((k, source))
    for k in range(1, cores):
        copy = rdma(down, down_block(g, t), td_send.at[k, 0], td_recv.at[k, 0], to("tp", t, cores, k))
        copy.start()
        sends.append(copy)

    for i in range(1, inner):
        copy = rdma(normed, block_of(tok, i), tok_send.at[i], tok_recv.at[i], ahead(0, i))
        copy.start()
        sends.append(copy)

    def beside(step):
        return {"fs": (z + step) * inner + y}

    def hop(o, step):
        source = normed if o in (0, outer) else block_of(tok, o * inner)
        n = (o + step) * inner
        return rdma(source, block_of(tok, n), hop_send.at[o + step if step > 0 else outer + o + step], tok_recv.at[n], beside(step))

    low, high = z > 0, z < outer - 1
    hops = []

    def move(o, step, when):
        pl.when(when)(lambda: hop(o, step).start())
        hops.append((o, step, when))

    move(0, 1, high)
    move(outer, -1, low)

    def up_copy(i):
        number = t * nseg + i
        shard, sg = lax.rem(number, shards), number // shards
        step = lax.rem(shard - f + shards, shards)
        src = up.at[:, pl.ds(pl.multiple_of(i * segment, segment), segment)]
        remote = rdma(src, up_block(g, f, sg), up_send.at[i], up_recv.at[sg, step], {"fs": shard})
        here = pltpu.make_async_copy(src, up_block(g, f, sg), up_recv.at[sg, 0])
        return shard == f, here, remote

    def start_up(j, carry):
        mine, here, remote = up_copy(lax.rem(f + j, nseg))
        pl.when(mine)(here.start)
        pl.when(jnp.logical_not(mine))(remote.start)
        return carry

    lax.fori_loop(0, nseg, start_up, 0)

    def pass_on(o):
        for n, when, step, more in ((o, z >= o, 1, high), (outer - o, z + o < outer, -1, low)):
            block = block_of(tok, n * inner)

            @pl.when(when)
            def _(n=n, step=step, block=block):
                rdma(block, block, tok_send.at[0], tok_recv.at[n * inner], beside(-step)).wait_recv()

            if 0 < n + step < outer:
                move(n, step, when & more)

            @pl.when(when)
            def _(n=n, block=block):
                for i in range(1, inner):
                    at = n * inner + i
                    rdma(block, block_of(tok, at), tok_send.at[at], tok_recv.at[at], ahead(0, i)).start()

    if outer > 1:
        pass_on(1)

    for sg in range(groups):
        def forward(sg=sg):
            def arrived(k, carry):
                shard = lax.rem(f + shards - k, shards)
                block = up_block(g, shard, sg)

                @pl.when(k == 0)
                def _():
                    pltpu.make_async_copy(block, block, up_recv.at[sg, 0]).wait()

                @pl.when(k > 0)
                def _():
                    rdma(block, block, up_send.at[0], up_recv.at[sg, k], {"fs": shard}).wait_recv()

                for d in range(1, groups):
                    rdma(block, block, gu_send.at[sg, d, k], gu_recv.at[sg, d, k],
                         to("gr", g, groups, d)).start()
                return carry

            lax.fori_loop(0, shards, arrived, 0)
            whole = up_group(g, sg)
            for c in range(1, cores):
                rdma(whole, whole, tu_send.at[sg, 0, c], tu_recv.at[sg, 0], to("tp", t, cores, c)).start()

        pl.when(owner(sg) == t)(forward)

    for o in range(2, outer):
        pass_on(o)

    for k, source in down_in:
        block = down_block(source, t)
        rdma(block, block, gd_send.at[k], gd_recv.at[k], {"gr": source}).wait_recv()
        for c in range(1, cores):
            copy = rdma(block, block, td_send.at[c, k], td_recv.at[c, k], to("tp", t, cores, c))
            copy.start()
            sends.append(copy)

    for sg in range(groups):
        def onward(sg=sg):
            for d in range(1, groups):
                source = lax.rem(g + groups - d, groups)

                def arrived(k, carry):
                    block = up_block(source, lax.rem(f + shards - k, shards), sg)
                    rdma(block, block, gu_send.at[sg, d, k], gu_recv.at[sg, d, k], {"gr": source}).wait()
                    for c in range(1, cores):
                        rdma(block, block, ou_send.at[sg, d, c, k], ou_recv.at[sg, d, k],
                             to("tp", t, cores, c)).start()
                    return carry

                lax.fori_loop(0, shards, arrived, 0)

        pl.when(owner(sg) == t)(onward)

    keep_down.wait()
    keep_tok.wait()
    for c in range(1, cores):
        core = lax.rem(t + cores - c, cores)
        for k in range(groups):
            block = down_block(lax.rem(g + groups - k, groups), core)
            rdma(block, block, td_send.at[c, k], td_recv.at[c, k], {"tp": core}).wait_recv()
    for sg in range(groups):
        def take(sg=sg):
            whole = up_group(g, sg)
            rdma(whole, whole, tu_send.at[sg, 0, 1], tu_recv.at[sg, 0], {"tp": owner(sg)}).wait_recv()
            for d in range(1, groups):
                def taken(k, carry):
                    block = up_block(lax.rem(g + groups - d, groups), lax.rem(f + shards - k, shards), sg)
                    rdma(block, block, tu_send.at[sg, 0, 1], ou_recv.at[sg, d, k],
                         {"tp": owner(sg)}).wait_recv()
                    return carry

                lax.fori_loop(0, shards, taken, 0)

        pl.when(owner(sg) != t)(take)

    width = su.shape[1]
    stack = inner * rows

    def near_copy(o, i):
        n = o * inner + i
        return rdma(block_of(part, n), block_of(got, n), part_send.at[n], part_recv.at[n], back(0, i))

    def far_copy(o):
        right = o > z
        step = jnp.where(right, 1, -1)
        last = jnp.where(right, o == outer - 1, o == 1)
        slot = jnp.where(last, jnp.where(right, 0, outer), o + step)
        return rdma(block_of(part, o * inner), block_of(far, slot), far_send.at[o], far_recv.at[slot],
                    beside(step))

    def far_arrived(slot, step):
        rdma(block_of(far, slot), block_of(far, slot), far_send.at[0], far_recv.at[slot],
             beside(step)).wait_recv()

    def compute(o):
        for i in range(1, inner):
            block = block_of(tok, o * inner + i)
            n = o * inner + i
            rdma(block, block, tok_send.at[n], tok_recv.at[n], back(0, i)).wait_recv()
        both = pl.ds(pl.multiple_of(o * stack, stack), stack)

        def first(n, carry):
            cols = pl.ds(pl.multiple_of(n * TILE, TILE), TILE)
            product = jnp.dot(tok[both, :], su[:, cols], preferred_element_type=jnp.float32)
            product = jnp.maximum(product, 0.0)
            hid[:, cols] = (product * product).astype(jnp.bfloat16)
            return carry

        lax.fori_loop(0, width // TILE, first, 0)

        def second(n, carry):
            cols = pl.ds(pl.multiple_of(n * TILE, TILE), TILE)
            product = jnp.dot(hid[...], sd[:, cols], preferred_element_type=jnp.float32)
            part[both, cols] = product.astype(jnp.bfloat16)
            return carry

        lax.fori_loop(0, depth // TILE, second, 0)
        for i in range(1, inner):
            near_copy(o, i).start()

    def gather(o):
        for i in range(1, inner):
            near_copy(o, i).wait()

    def add(o):
        gather(o)

        def sum_up(passed):
            def chunk(r, carry):
                at = pl.multiple_of(r * 16, 16)
                mine = pl.ds(pl.multiple_of(o * stack + at, 16), 16)
                value = part[mine, :].astype(jnp.float32)
                for i in range(1, inner):
                    near = pl.ds(pl.multiple_of(o * stack + i * rows + at, 16), 16)
                    value += got[near, :].astype(jnp.float32)
                if passed:
                    value += far[pl.ds(pl.multiple_of(o * rows + at, 16), 16), :].astype(jnp.float32)
                part[mine, :] = value.astype(jnp.bfloat16)
                return carry

            lax.fori_loop(0, rows // 16, chunk, 0)

        right = o > z
        passed = (right & low) | (jnp.logical_not(right) & high)

        @pl.when(passed)
        def _():
            far_arrived(o, jnp.where(right, -1, 1))
            sum_up(True)

        pl.when(jnp.logical_not(passed))(lambda: sum_up(False))
        far_copy(o).start()

    order = []
    left_end, right_end = z * 0, z * 0 + outer - 1
    for _ in range(outer):
        take_left = z - left_end > right_end - z
        owner_z = jnp.where(take_left, left_end, right_end)
        order.append(lax.rem(z - owner_z + outer, outer))
        left_end = jnp.where(take_left, left_end + 1, left_end)
        right_end = jnp.where(take_left, right_end, right_end - 1)

    for o in order:
        compute(o)
    for o in order[:-1]:
        add(o)
    gather(0)
    pl.when(low)(lambda: far_arrived(0, -1))
    pl.when(high)(lambda: far_arrived(outer, 1))

    def total(ends):
        def chunk(r, carry):
            at = pl.multiple_of(r * 16, 16)
            value = part[pl.ds(at, 16), :].astype(jnp.float32)
            for i in range(1, inner):
                value += got[pl.ds(pl.multiple_of(i * rows + at, 16), 16), :].astype(jnp.float32)
            for end in ends:
                value += far[pl.ds(pl.multiple_of(end * rows + at, 16), 16), :].astype(jnp.float32)
            served[pl.ds(at, 16), :] = value.astype(jnp.bfloat16)
            return carry

        lax.fori_loop(0, rows // 16, chunk, 0)

    pl.when(low & high)(lambda: total((0, outer)))
    pl.when(low & jnp.logical_not(high))(lambda: total((0,)))
    pl.when(jnp.logical_not(low) & high)(lambda: total((outer,)))
    pl.when(jnp.logical_not(low | high))(lambda: total(()))

    for o, step, when in hops:
        pl.when(when)(lambda o=o, step=step: hop(o, step).wait_send())
    for n in range(inner, shards):
        if n % inner:
            block = block_of(tok, n)
            rdma(block, block, tok_send.at[n], tok_recv.at[n], ahead(0, n % inner)).wait_send()
    for o in range(1, outer):
        far_copy(o).wait_send()
    for copy in sends:
        copy.wait_send()

    def end_up(j, carry):
        mine, here, remote = up_copy(j)
        pl.when(jnp.logical_not(mine))(remote.wait_send)
        return carry

    lax.fori_loop(0, nseg, end_up, 0)
    for sg in range(groups):
        def end(sg=sg):
            whole = up_group(g, sg)
            for c in range(1, cores):
                rdma(whole, whole, tu_send.at[sg, 0, c], tu_recv.at[sg, 0],
                     to("tp", t, cores, c)).wait_send()
            for d in range(1, groups):
                def left(k, carry):
                    block = up_block(lax.rem(g + groups - d, groups), lax.rem(f + shards - k, shards), sg)
                    for c in range(1, cores):
                        rdma(block, block, ou_send.at[sg, d, c, k], ou_recv.at[sg, d, k],
                             to("tp", t, cores, c)).wait_send()
                    return carry

                lax.fori_loop(0, shards, left, 0)

        pl.when(owner(sg) == t)(end)


def body(tokens, norm_gain, up_weight, down_weight):
    groups, shards, cores = (lax.axis_size(a) for a in ("gr", "fs", "tp"))
    segment = down_weight.shape[0]
    up = (norm_gain[:, None] * up_weight).astype(jnp.bfloat16)
    down = down_weight.astype(jnp.bfloat16)
    values = tokens.astype(jnp.float32)
    normed = (values * lax.rsqrt(jnp.mean(values * values, axis=1, keepdims=True) + 1e-06)).astype(
        jnp.bfloat16
    )
    rows, depth = tokens.shape
    inner = inner_size(shards)
    nseg = up.shape[1] // segment
    width = groups * segment
    bf = jnp.bfloat16
    dma = pltpu.SemaphoreType.DMA
    vmem = pl.BlockSpec(memory_space=pltpu.VMEM)
    return pl.pallas_call(
        functools.partial(kernel, (groups, shards, cores)),
        out_shape=(
            jax.ShapeDtypeStruct((rows, depth), bf),
            jax.ShapeDtypeStruct((depth, width), bf),
            jax.ShapeDtypeStruct((width, depth), bf),
        ),
        in_specs=[vmem] * 3,
        out_specs=(vmem, vmem, vmem),
        scratch_shapes=[
            pltpu.VMEM((shards * rows, depth), bf),
            pltpu.VMEM((inner * rows, width), bf),
            pltpu.VMEM((shards * rows, depth), bf),
            pltpu.VMEM((shards * rows, depth), bf),
            pltpu.VMEM(((shards // inner + 1) * rows, depth), bf),
            dma((nseg,)), dma((groups, shards)),
            dma((groups, groups, shards)), dma((groups, groups, shards)),
            dma((groups, groups, cores)), dma((groups, groups)),
            dma((groups,)), dma((groups,)),
            dma((cores, groups)), dma((cores, groups)),
            dma((shards,)), dma((shards,)),
            dma((shards,)), dma((shards,)),
            dma((shards // inner,)), dma((shards // inner + 1,)), dma((2 * (shards // inner),)),
            dma((groups, groups, cores, shards)), dma((groups, groups, shards)),
            dma((2,)),
        ],
        compiler_params=pltpu.CompilerParams(
            collective_id=0, has_side_effects=True, vmem_limit_bytes=34 * 1024 * 1024
        ),
        name="serve",
    )(normed, up, down)


def solution(mesh):
    return jax.shard_map(
        body,
        mesh=mesh,
        in_specs=(
            P(("gr", "fs", "tp"), None),
            P(("gr", "fs")),
            P(("gr", "fs"), "tp"),
            P(("gr", "fs"), "tp"),
        ),
        out_specs=(P(("gr", "fs", "tp"), None), P(None, "fs"), P("fs", None)),
        check_vma=False,
    )
```
